256 devices in a mesh: ep: 64 (over z, x, core), tp: 4 (over y).
Axes of the slice: x: 4, y: 4, z: 8, core: 2. Of those that a mesh axis runs over, the one named last changes fastest.
Arguments:
- queries: bfloat16 [16384, 8, 128], P('ep', 'tp'), may hold values from -256 to 256
- keys: bfloat16 [16384, 4, 128], P('ep', 'tp'), may hold values from -8 to 8
- values: bfloat16 [16384, 4, 128], P('ep', 'tp'), may hold values from -6 to 6
- attn_lambda: float32 [8], P('tp'), may hold values from 0.3 to 0.8
- head_gain: float32 [128], replicated, may hold values from 0.1 to 1.9
- w_out: bfloat16 [1024, 2048], replicated, may hold values from -0.1875 to 0.1875
- moe_rows: bfloat16 [32768, 2048], P('ep'), may hold values from -6 to 6
- moe_gain: float32 [2048], replicated, may hold values from 0.1 to 1.9
- routes: int32 [32768, 2], P('ep'), may hold values from 0 to 63, all different within a row; in each aligned block of 128 rows (0 to 127, 128 to 255, ...) at most 8 rows name the same one
- route_weights: float32 [32768, 2], P('ep'), may hold values from 0.1 to 1
- w_gate: bfloat16 [64, 2048, 1024], P('ep', None, 'tp'), may hold values from -0.125 to 0.125
- w_up: bfloat16 [64, 2048, 1024], P('ep', None, 'tp'), may hold values from -0.125 to 0.125
- w_down: bfloat16 [64, 1024, 2048], P('ep', 'tp'), may hold values from -0.1875 to 0.1875
Outputs:
- mixer_out: bfloat16 [16384, 2048], P(('ep', 'tp'))
- moe_out: bfloat16 [32768, 2048], P(('ep', 'tp'))
The draws below stay inside these ranges and needn't reach their ends.
Inputs may be any that keep to these rules, and one draw needn't show every extreme that they name: `routes`: each row names 2 different experts. In each aligned block of 128 rows (the rows of moe_out that one device holds) no expert is named by more than 8 rows, a bound that some block reaches.
All inputs are finite; a program needn't handle non-finite values.
Results may differ from the reference program's by a relative error of at most 0.011.
Values may be sent and summed in bfloat16 or wider, within the bound.
No kernel may reach another device: no remote copies, remote signals or barrier semaphores. Data moves between devices by JAX's collectives and lax.ppermute only.
A program may use at most 128 MiB of HBM per device.

```python
import math
import jax
import jax.numpy as jnp
import numpy as np
from jax import lax

D = 2048
HQ = 8
KVH = 4
HEAD = 64
VDIM = 128
FF = 1024
TOPK = 2
MOE_DEV = 128
EXPERTS = 64
CAP = 8
ATT_TOKENS = 16384
MOE_TOKENS = 32768
N_EP = 64
N_TP = 4


def pair_draw(key):
    spread = 1.75 ** 0.5
    base_q = jax.random.truncated_normal(jax.random.fold_in(key, 101), -4.5, 4.5, (ATT_TOKENS, HQ, 2, HEAD), jnp.float32) * spread
    base_k = jax.random.truncated_normal(jax.random.fold_in(key, 102), -4.5, 4.5, (ATT_TOKENS, KVH, 2, HEAD), jnp.float32) * spread
    return (base_q.reshape(ATT_TOKENS, HQ, 2 * HEAD), base_k.reshape(ATT_TOKENS, KVH, 2 * HEAD))


def draw_queries(key, part):
    return pair_draw(key)[0].astype(jnp.bfloat16)


def draw_keys(key, part):
    return pair_draw(key)[1].astype(jnp.bfloat16)


def steps_of(key, shape, shards, low, high):
    factor_of = 1.0
    for dim, blocks in shards:
        steps = jax.random.uniform(jax.random.fold_in(jax.random.fold_in(key, 6), dim), (blocks,), jnp.float32, low / len(shards), high / len(shards))
        factor_of = factor_of * jnp.repeat(jnp.exp(steps), shape[dim] // blocks).reshape((-1,) + (1,) * (len(shape) - 1 - dim))
    return factor_of


def deal_out(key, own, number, rows, number_of, top, limit, slope):
    order = jax.random.permutation(key, number_of)
    heavy_load, ordinary = load_shares(number_of, rows * top, limit, slope, True), load_shares(number_of, rows * top, limit, slope, False)
    places = jnp.arange(number_of)

    def named(tallies, offset_by):
        used = int((tallies > 0).sum())
        fixed = max(1, used // 4)
        moved = fixed + (places - fixed + offset_by * (used - fixed)) % max(1, number_of - fixed)
        return jnp.zeros((number_of,), jnp.int32).at[order[jnp.where(places < fixed, places, moved)]].set(jnp.asarray(tallies, jnp.int32))

    tallies = jnp.where(number % 4 == 0, named(heavy_load, number // 4), named(ordinary, number - number // 4 - 1))
    mixed = jax.random.permutation(jax.random.fold_in(own, 3), number_of)
    source_of, taker = mixed[0:number_of // 2 * 2:2], mixed[1:number_of // 2 * 2:2]
    slack = jnp.minimum(tallies[source_of] - 1, limit - tallies[taker]) // 2
    slack = jnp.where((source_of == order[0]) | (taker == order[0]) | (tallies[taker] == 0), 0, jnp.maximum(slack, 0))
    moved = jax.random.randint(jax.random.fold_in(own, 4), (number_of // 2,), 0, 1 << 20) % (slack + 1)
    tallies = tallies.at[source_of].add(-moved).at[taker].add(moved)
    members = jnp.searchsorted(jnp.cumsum(tallies), jnp.arange(rows * top), side="right").astype(jnp.int32)
    table = members.reshape(top, rows).T
    table = table[jax.random.permutation(jax.random.fold_in(own, 1), rows)]
    offset_by = jax.random.randint(jax.random.fold_in(own, 2), (rows, 1), 0, top)
    return jnp.take_along_axis(table, (jnp.arange(top)[None, :] + offset_by) % top, axis=1)


def load_shares(amount, total, bound, lean, full):
    weights = [(1 << 20) // math.isqrt(standing ** lean) + 1 for standing in range(1, amount + 1)]
    largest = bound if full else min(bound, max(-(-total // amount), total * weights[0] // sum(weights)))
    least = 1 if total - largest >= amount - 1 else 0
    counts, spare = [largest] + [least] * (amount - 1), total - largest - least * (amount - 1)
    while spare > 0:
        free = [i for i in range(1, amount) if counts[i] < largest] or [i for i in range(1, amount) if counts[i] < bound]
        pool, budget = sum([weights[i] for i in free]), spare
        for i in free:
            extra = min(bound - counts[i], max(1, budget * weights[i] // pool), spare)
            counts[i] = counts[i] + extra
            spare = spare - extra
    return np.array(counts)


def normal_values(rng, extent, deviation, limit, split=(), kind=jnp.bfloat16):
    entries = deviation * jax.random.normal(rng, extent, jnp.float32)
    if split:
        entries = entries * steps_of(rng, extent, split, -0.22, 0.18)
    return jnp.clip(entries, -limit, limit).astype(kind)


def setup_inputs(seed: int = 0) -> dict:
    streams_of = jax.random.split(jax.random.key(seed), 14)
    queries = draw_queries(jax.random.fold_in(streams_of[13], 71), 0)
    keys = draw_keys(jax.random.fold_in(streams_of[13], 71), 0)
    values = normal_values(streams_of[2], (ATT_TOKENS, KVH, VDIM), 1.0, 6.0, ((0, 64), (1, 4)))
    attn_lambda = jnp.clip(0.3 + 0.5 * jax.random.uniform(streams_of[3], (HQ,), jnp.float32) ** steps_of(streams_of[3], (HQ,), ((0, 4),), -0.2, 0.2), 0.3, 0.8)
    head_gain = jnp.clip(1.0 + 0.18 * jax.random.normal(streams_of[4], (VDIM,), jnp.float32), 0.1, 1.9)
    w_out = normal_values(streams_of[5], (HQ * VDIM, D), (HQ * VDIM) ** -0.5, 0.1875)
    moe_rows = normal_values(streams_of[6], (MOE_TOKENS, D), 1.0, 6.0, ((0, 64),))
    moe_gain = jnp.clip(1.0 + 0.18 * jax.random.normal(streams_of[7], (D,), jnp.float32), 0.1, 1.9)
    routes_keys = jax.random.split(jax.random.fold_in(streams_of[8], 1), MOE_TOKENS // MOE_DEV)
    routes_turns = jax.random.permutation(jax.random.fold_in(streams_of[8], 3), MOE_TOKENS // MOE_DEV)
    routes = jax.vmap(lambda own, number: deal_out(jax.random.fold_in(streams_of[8], 2), own, number, MOE_DEV, EXPERTS, TOPK, CAP, 1))(routes_keys, routes_turns).reshape((MOE_TOKENS, TOPK))
    route_weights = jnp.clip(0.1 + 0.9 * jax.random.uniform(streams_of[9], (MOE_TOKENS, TOPK), jnp.float32) ** steps_of(streams_of[9], (MOE_TOKENS, TOPK), ((0, 64),), -0.2, 0.2), 0.1, 1.0)
    w_gate = normal_values(streams_of[10], (EXPERTS, D, FF), D ** -0.5, 0.125, ((0, 64), (2, 4)))
    w_up = normal_values(streams_of[11], (EXPERTS, D, FF), D ** -0.5, 0.125, ((0, 64), (2, 4)))
    w_down = normal_values(streams_of[12], (EXPERTS, FF, D), FF ** -0.5, 0.1875, ((0, 64), (1, 4)))
    return dict(queries=queries, keys=keys, values=values, attn_lambda=attn_lambda, head_gain=head_gain, w_out=w_out, moe_rows=moe_rows, moe_gain=moe_gain, routes=routes, route_weights=route_weights, w_gate=w_gate, w_up=w_up, w_down=w_down)


EPSILON = 1e-06
MASKED = -1e+30

def reference(queries, keys, values, attn_lambda, head_gain, w_out, moe_rows, moe_gain, routes, route_weights, w_gate, w_up, w_down):
    length = queries.shape[0]
    per_key = HQ // KVH
    key_all = jnp.repeat(keys.astype(jnp.float32).reshape(length, KVH, 2, HEAD), per_key, axis=1)
    value_all = jnp.repeat(values.astype(jnp.float32), per_key, axis=1)
    block_len = math.gcd(length, 256)
    block_count = length // block_len
    query_all = queries.astype(jnp.float32).reshape(block_count, block_len, HQ, 2, HEAD)
    key_pos = jnp.arange(length, dtype=jnp.int32)

    def one_block(inputs):
        query_blk, block_index = inputs
        query_pos = block_index * block_len + jnp.arange(block_len, dtype=jnp.int32)
        scores = jnp.einsum('qhmd,khmd->hmqk', query_blk, key_all) * HEAD ** (-0.5)
        allowed = key_pos[None, :] <= query_pos[:, None]
        scores = jnp.where(allowed, scores, MASKED)
        row_max = lax.optimization_barrier(jnp.max(scores, axis=-1, keepdims=True))
        weights = jnp.exp(scores - row_max)
        totals = lax.optimization_barrier(jnp.sum(weights, axis=-1))
        rounded = lax.optimization_barrier(weights.astype(jnp.bfloat16)).astype(jnp.float32)
        numerator = jnp.einsum('hmqk,khv->hmqv', rounded, value_all)
        ratios = numerator / totals[..., None]
        head_out = ratios[:, 0] - attn_lambda[:, None, None] * ratios[:, 1]
        inv_rms = lax.rsqrt(lax.optimization_barrier(jnp.mean(head_out * head_out, axis=-1, keepdims=True)) + EPSILON)
        normed_heads = (head_out * inv_rms * head_gain).astype(jnp.bfloat16)
        return jnp.transpose(normed_heads, (1, 0, 2)).reshape(block_len, HQ * VDIM)
    attn_rows = lax.map(one_block, (query_all, jnp.arange(block_count, dtype=jnp.int32)))
    attn_rows = attn_rows.reshape(length, HQ * VDIM)
    mixer_out = jnp.dot(attn_rows, w_out, preferred_element_type=jnp.float32).astype(jnp.bfloat16)
    rows_f = moe_rows.astype(jnp.float32)
    normed = (rows_f * lax.rsqrt(lax.optimization_barrier(jnp.mean(rows_f * rows_f, axis=-1, keepdims=True)) + EPSILON) * moe_gain).astype(jnp.bfloat16)
    tokens = moe_rows.shape[0]
    pairs = tokens * TOPK
    flat_ids = routes.reshape(-1).astype(jnp.int32)
    matches = (flat_ids[:, None] == jnp.arange(EXPERTS, dtype=jnp.int32)[None, :]).astype(jnp.int32)
    earlier = jnp.cumsum(matches, axis=0) - matches
    position = lax.optimization_barrier(jnp.sum(earlier * matches, axis=1)).astype(jnp.int32)
    slot_total = N_EP * N_TP * CAP
    pair_table = jnp.full((EXPERTS, slot_total), pairs, dtype=jnp.int32)
    pair_table = pair_table.at[flat_ids, position].set(jnp.arange(pairs, dtype=jnp.int32))
    token_table = jnp.where(pair_table < pairs, pair_table // TOPK, tokens).astype(jnp.int32)
    weight_flat = jnp.concatenate([route_weights.reshape(-1), jnp.zeros((1,), jnp.float32)])
    weight_table = weight_flat[pair_table]
    padded = jnp.concatenate([normed, jnp.zeros((1, D), jnp.bfloat16)], axis=0)
    group_width = FF // N_TP

    def one_expert(accumulated, inputs):
        token_row, weight_row, gate_w, up_w, down_w = inputs
        chosen = padded[token_row]
        gate_out = jnp.dot(chosen, gate_w, preferred_element_type=jnp.float32)
        up_out = jnp.dot(chosen, up_w, preferred_element_type=jnp.float32)
        hidden = (jax.nn.silu(gate_out) * up_out).astype(jnp.bfloat16)
        partials = jnp.einsum('stf,tfd->tsd', hidden.reshape(slot_total, N_TP, group_width).astype(jnp.float32), down_w.reshape(N_TP, group_width, D).astype(jnp.float32))
        partials = lax.optimization_barrier(partials.astype(jnp.bfloat16)).astype(jnp.float32)
        expert_out = lax.optimization_barrier(lax.optimization_barrier(jnp.sum(partials, axis=0)).astype(jnp.bfloat16)).astype(jnp.float32)
        accumulated = accumulated.at[token_row].add(weight_row[:, None] * expert_out)
        return (accumulated, None)
    start_total = jnp.zeros((tokens + 1, D), jnp.float32)
    accumulated, unused = lax.scan(one_expert, start_total, (token_table, weight_table, w_gate, w_up, w_down))
    moe_out = accumulated[:tokens].astype(jnp.bfloat16)
    return (mixer_out, moe_out)
```

```python
import functools

import jax
import jax.numpy as jnp
from jax import lax
from jax.experimental import pallas as pl
from jax.experimental.pallas import tpu as pltpu
from jax.sharding import PartitionSpec as P


EPSILON = 1e-06
MASKED = -1e30
KEY_BLOCK = 1024


def attention_body(place_ref, lam_ref, q_ref, kv_ref, gain_ref, out_ref, qs_ref, max_ref, acc_ref, *, heads, dim):
    rows = q_ref.shape[0]
    width = 2 * dim
    first = place_ref[0] * rows
    lane = lax.broadcasted_iota(jnp.int32, (rows, width), 1)
    for h in range(heads):
        q_h = q_ref[:, h * width : (h + 1) * width] * jnp.bfloat16(dim**-0.5)
        for m in range(2):
            qs_ref[2 * h + m] = jnp.where((lane >= m * dim) & (lane < (m + 1) * dim), q_h, jnp.bfloat16(0))
    max_ref[...] = jnp.full_like(max_ref, MASKED)
    acc_ref[...] = jnp.zeros_like(acc_ref)

    def visit(block, masked):
        start = pl.multiple_of(block * KEY_BLOCK, KEY_BLOCK)
        key_blk = kv_ref[pl.ds(start, KEY_BLOCK), :width]
        value_blk = kv_ref[pl.ds(start, KEY_BLOCK), width:]
        value_ones = jnp.concatenate([value_blk, jnp.ones_like(value_blk)], axis=1)
        for g in range(2 * heads):
            scores = lax.dot_general(
                qs_ref[g], key_blk, (((1,), (1,)), ((), ())), preferred_element_type=jnp.float32
            )
            if masked:
                key_pos = start + lax.broadcasted_iota(jnp.int32, scores.shape, 1)
                query_pos = first + lax.broadcasted_iota(jnp.int32, scores.shape, 0)
                scores = jnp.where(key_pos <= query_pos, scores, MASKED)
            old_max = max_ref[g]
            new_max = jnp.maximum(old_max, jnp.max(scores, axis=1, keepdims=True))
            shrink = jnp.exp(old_max - new_max)
            weights = jnp.exp(scores - new_max[:, :1]).astype(jnp.bfloat16)
            part = jnp.dot(weights, value_ones, preferred_element_type=jnp.float32)
            acc_ref[g] = acc_ref[g] * jnp.concatenate([shrink, shrink], axis=1) + part
            max_ref[g] = new_max

    full_blocks = first // KEY_BLOCK

    @pl.loop(0, full_blocks)
    def _(block):
        visit(block, False)

    visit(full_blocks, True)
    for h in range(heads):
        one, two = acc_ref[2 * h], acc_ref[2 * h + 1]
        head_out = one[:, :width] / one[:, width:] - lam_ref[h] * (two[:, :width] / two[:, width:])
        mean_sq = jnp.mean(head_out * head_out, axis=1, keepdims=True)
        out_ref[:, h * width : (h + 1) * width] = (
            head_out * lax.rsqrt(mean_sq + EPSILON) * gain_ref[...]
        ).astype(jnp.bfloat16)


def attention(queries, kv, attn_lambda, head_gain, place):
    rows, heads, width = queries.shape
    maps = 2 * heads
    keys = kv.shape[0]
    return pl.pallas_call(
        functools.partial(attention_body, heads=heads, dim=width // 2),
        out_shape=jax.ShapeDtypeStruct((rows, heads * width), jnp.bfloat16),
        in_specs=[
            pl.BlockSpec(memory_space=pltpu.SMEM),
            pl.BlockSpec(memory_space=pltpu.SMEM),
            pl.BlockSpec(memory_space=pltpu.VMEM),
            pl.BlockSpec(memory_space=pltpu.VMEM),
            pl.BlockSpec(memory_space=pltpu.VMEM),
        ],
        out_specs=pl.BlockSpec(memory_space=pltpu.VMEM),
        scratch_shapes=[
            pltpu.VMEM((maps, rows, width), jnp.bfloat16),
            pltpu.VMEM((maps, rows, width), jnp.float32),
            pltpu.VMEM((maps, rows, 2 * width), jnp.float32),
        ],
        cost_estimate=pl.CostEstimate(
            flops=maps * rows * keys * 3 * width * 2,
            bytes_accessed=keys * 2 * width * 2,
            transcendentals=maps * rows * keys,
        ),
        compiler_params=pltpu.CompilerParams(vmem_limit_bytes=32 * 1024 * 1024),
        name="attention",
    )(
        place.reshape(1),
        attn_lambda,
        queries.reshape(rows, heads * width),
        kv,
        head_gain.reshape(1, -1),
    )


def down_body(*refs, hiddens):
    hidden = jnp.concatenate([ref[...] for ref in refs[:hiddens]], axis=1)
    weights = jnp.concatenate([ref[...] for ref in refs[hiddens:-1]], axis=0)
    refs[-1][...] = jnp.dot(hidden, weights, preferred_element_type=jnp.float32).astype(jnp.bfloat16)


def down_product(hidden, weights):
    rows = hidden[0].shape[0]
    width = weights[0].shape[1]
    cols = width // 4
    return pl.pallas_call(
        functools.partial(down_body, hiddens=len(hidden)),
        grid=(width // cols,),
        out_shape=jax.ShapeDtypeStruct((rows, width), jnp.bfloat16),
        in_specs=[pl.BlockSpec(h.shape, lambda n: (0, 0)) for h in hidden]
        + [pl.BlockSpec((w.shape[0], cols), lambda n: (0, n)) for w in weights],
        out_specs=pl.BlockSpec((rows, cols), lambda n: (0, n)),
        cost_estimate=pl.CostEstimate(
            flops=2 * rows * width * sum(w.shape[0] for w in weights),
            bytes_accessed=4 * rows * width,
            transcendentals=0,
        ),
        name="down_product",
    )(*hidden, *weights)


def ring(size, step):
    return [(i, (i + step) % size) for i in range(size)]


def local(
    queries,
    keys,
    values,
    attn_lambda,
    head_gain,
    w_out,
    moe_rows,
    moe_gain,
    routes,
    route_weights,
    w_gate,
    w_up,
    w_down,
):
    tp_count = lax.axis_size("tp")
    tp_id = lax.axis_index("tp")
    experts = lax.axis_size("ep")
    positions, _, _ = queries.shape
    model_width = moe_rows.shape[1]
    dev_rows = moe_rows.shape[0] // tp_count
    top_count = routes.shape[1]
    capacity = max(2, 2 * dev_rows * top_count // experts)
    slots = experts * capacity
    up_ring, down_ring = ring(tp_count, 1), ring(tp_count, -1)

    gate, up = w_gate[0], w_up[0]
    half = w_down.shape[1] // 2
    down = w_down[0]
    downs = [down[:half], down[half:]]

    def send(x, way):
        return lax.ppermute(x, "tp", way)

    gate_a, gate_b = send(gate, up_ring), send(gate, down_ring)
    up_a, up_b = send(up, up_ring), send(up, down_ring)
    gate_c, up_c = send(gate_a, up_ring), send(up_b, down_ring)
    down_parts = []
    for c, x in enumerate(downs):
        near_a, near_b = send(x, up_ring), send(x, down_ring)
        far = send(near_a, up_ring) if c == 0 else send(near_b, down_ring)
        down_parts.append((near_a, near_b, far))

    kv = jnp.concatenate([keys.reshape(positions, -1), values.reshape(positions, -1)], axis=1)
    kv_all = lax.all_gather(kv, "ep", axis=0, tiled=True)

    own_routes = lax.dynamic_slice_in_dim(routes, tp_id * dev_rows, dev_rows, 0)
    own_weights = lax.dynamic_slice_in_dim(route_weights, tp_id * dev_rows, dev_rows, 0)
    rows_f = lax.dynamic_slice_in_dim(moe_rows, tp_id * dev_rows, dev_rows, 0).astype(jnp.float32)
    mean_sq = jnp.mean(rows_f * rows_f, axis=-1, keepdims=True)
    normed = (rows_f * lax.rsqrt(mean_sq + EPSILON) * moe_gain).astype(jnp.bfloat16)
    flat_ids = own_routes.reshape(-1)
    order = lax.iota(jnp.int32, flat_ids.shape[0])
    same = (flat_ids[:, None] == flat_ids[None, :]) & (order[None, :] < order[:, None])
    slot_ids = jnp.sum(same.astype(jnp.int32), axis=1)
    place = (flat_ids * capacity + slot_ids).reshape(dev_rows, top_count)
    slot_range = lax.iota(jnp.int32, slots)
    taken = slot_range[:, None] == place[:, 0][None, :]
    for k in range(1, top_count):
        taken = taken | (slot_range[:, None] == place[:, k][None, :])
    outgoing = jnp.dot(taken.astype(jnp.bfloat16), normed, preferred_element_type=jnp.float32).astype(jnp.bfloat16)
    arrived = lax.all_to_all(
        outgoing.reshape(experts, capacity, model_width), "ep", split_axis=0, concat_axis=0, tiled=True
    ).reshape(slots, model_width)

    def hidden_of(g, u):
        gate_out = jnp.dot(arrived, g, preferred_element_type=jnp.float32)
        up_out = jnp.dot(arrived, u, preferred_element_type=jnp.float32)
        return (jax.nn.silu(gate_out) * up_out).astype(jnp.bfloat16)

    hidden = []
    for g, u in ((gate, up), (gate_a, up_a), (gate_b, up_b), (gate_c, up_c)):
        hidden.append(hidden_of(g, u))

    hit = [(slot_range[None, :] == place[:, k][:, None]).astype(jnp.float32) for k in range(top_count)]
    mix = sum(own_weights[:, k : k + 1] * hit[k] for k in range(top_count))
    mix_hi = mix.astype(jnp.bfloat16)
    mix_lo = (mix - mix_hi.astype(jnp.float32)).astype(jnp.bfloat16)
    near_a, near_b, far = zip(*down_parts)
    out = down_product(hidden, [down, *near_a, *near_b, *far])
    returned = lax.all_to_all(
        out.reshape(experts, capacity, -1), "ep", split_axis=0, concat_axis=0, tiled=True
    ).reshape(slots, -1)
    moe_out = (
        jnp.dot(mix_hi, returned, preferred_element_type=jnp.float32)
        + jnp.dot(mix_lo, returned, preferred_element_type=jnp.float32)
    ).astype(jnp.bfloat16)

    attn_rows = attention(queries, kv_all, attn_lambda, head_gain, lax.axis_index("ep"))
    block = positions // tp_count
    head_width = attn_rows.shape[1]
    mixer_f = jnp.zeros((block, model_width), jnp.float32)
    for step in range(tp_count):
        piece = lax.dynamic_slice_in_dim(attn_rows, (tp_id + step) % tp_count * block, block, 0)
        if step:
            piece = send(piece, ring(tp_count, step))
        w_rows = lax.dynamic_slice_in_dim(w_out, (tp_id - step) % tp_count * head_width, head_width, 0)
        mixer_f = mixer_f + jnp.dot(piece, w_rows, preferred_element_type=jnp.float32)
    mixer_out = mixer_f.astype(jnp.bfloat16)
    return (mixer_out, moe_out)


def solution(mesh):
    return jax.shard_map(
        local,
        mesh=mesh,
        in_specs=(
            P("ep", "tp", None),
            P("ep", "tp", None),
            P("ep", "tp", None),
            P("tp"),
            P(),
            P(),
            P("ep", None),
            P(),
            P("ep", None),
            P("ep", None),
            P("ep", None, "tp"),
            P("ep", None, "tp"),
            P("ep", "tp", None),
        ),
        out_specs=(P(("ep", "tp"), None), P(("ep", "tp"), None)),
        check_vma=False,
    )
```

```python
import functools

import jax
import jax.numpy as jnp
from jax import lax
from jax.experimental import pallas as pl
from jax.experimental.pallas import tpu as pltpu
from jax.sharding import PartitionSpec as P


EPSILON = 1e-06
MASKED = -1e30
EP_SIZES = (8, 4, 2)


def attention_body(place_ref, lam_ref, q_ref, gain_ref, *refs, heads, dim):
    _, x_size, cores = EP_SIZES
    count = x_size * cores
    piece_refs = refs[:count]
    out_ref, kv_ref, sems, qs_ref, max_ref, acc_ref = refs[count:]
    copies = [pltpu.make_async_copy(piece_refs[i], kv_ref.at[i], sems.at[i]) for i in range(count)]
    for copy in copies:
        copy.start()
    rows = q_ref.shape[0]
    width = 2 * dim
    me = place_ref[0]
    core = me % cores
    x = (me // cores) % x_size
    z = me // (cores * x_size)
    lane = lax.broadcasted_iota(jnp.int32, (rows, width), 1)
    for h in range(heads):
        q_h = q_ref[:, h * width : (h + 1) * width] * jnp.bfloat16(dim**-0.5)
        for m in range(2):
            qs_ref[2 * h + m] = jnp.where((lane >= m * dim) & (lane < (m + 1) * dim), q_h, jnp.bfloat16(0))
    max_ref[...] = jnp.full_like(max_ref, MASKED)
    acc_ref[...] = jnp.zeros_like(acc_ref)
    for copy in copies:
        copy.wait()

    def visit(pieces, offset, places):
        key_blk = jnp.concatenate([kv_ref[p, pl.ds(offset, rows), :width] for p in pieces], axis=0)
        value_blk = jnp.concatenate([kv_ref[p, pl.ds(offset, rows), width:] for p in pieces], axis=0)
        value_ones = jnp.concatenate([value_blk, jnp.ones_like(value_blk)], axis=1)
        for g in range(2 * heads):
            scores = lax.dot_general(
                qs_ref[g], key_blk, (((1,), (1,)), ((), ())), preferred_element_type=jnp.float32
            )
            if places is not None:
                shape = (rows, rows)
                query_pos = me * rows + lax.broadcasted_iota(jnp.int32, shape, 0)
                key_pos = lax.broadcasted_iota(jnp.int32, shape, 1)
                first_key = jnp.concatenate([place * rows + key_pos for place in places], axis=1)
                allowed = first_key <= jnp.concatenate([query_pos] * len(places), axis=1)
                scores = jnp.where(allowed, scores, MASKED)
            old_max = max_ref[g]
            new_max = jnp.maximum(old_max, jnp.max(scores, axis=1, keepdims=True))
            shrink = jnp.exp(old_max - new_max)
            spread_max = jnp.concatenate([new_max] * (scores.shape[1] // width), axis=1)
            weights = jnp.exp(scores - spread_max).astype(jnp.bfloat16)
            part = jnp.dot(weights, value_ones, preferred_element_type=jnp.float32)
            acc_ref[g] = acc_ref[g] * jnp.concatenate([shrink, shrink], axis=1) + part
            max_ref[g] = new_max

    @pl.loop(0, x + 1)
    def _(dx):
        first = (z * x_size + x - dx) * cores
        visit((dx, x_size + dx), 0, (first + core, first + 1 - core))

    @pl.loop(0, z * cores)
    def _(step):
        offset = pl.multiple_of((step // cores + 1) * rows, rows)
        first = step % cores * x_size
        visit([first + dx for dx in range(x_size)], offset, None)

    for h in range(heads):
        one, two = acc_ref[2 * h], acc_ref[2 * h + 1]
        head_out = one[:, :width] / one[:, width:] - lam_ref[h] * (two[:, :width] / two[:, width:])
        mean_sq = jnp.mean(head_out * head_out, axis=1, keepdims=True)
        out_ref[:, h * width : (h + 1) * width] = (
            head_out * lax.rsqrt(mean_sq + EPSILON) * gain_ref[...]
        ).astype(jnp.bfloat16)


def attention(queries, pieces, attn_lambda, head_gain, place):
    rows, heads, width = queries.shape
    maps = 2 * heads
    count = len(pieces)
    keys = count * pieces[0].shape[0]
    return pl.pallas_call(
        functools.partial(attention_body, heads=heads, dim=width // 2),
        out_shape=jax.ShapeDtypeStruct((rows, heads * width), jnp.bfloat16),
        in_specs=[pl.BlockSpec(memory_space=pltpu.SMEM)] * 2
        + [pl.BlockSpec(memory_space=pltpu.VMEM)] * 2
        + [pl.BlockSpec(memory_space=pltpu.HBM)] * count,
        out_specs=pl.BlockSpec(memory_space=pltpu.VMEM),
        scratch_shapes=[
            pltpu.VMEM((count, *pieces[0].shape), jnp.bfloat16),
            pltpu.SemaphoreType.DMA((count,)),
            pltpu.VMEM((maps, rows, width), jnp.bfloat16),
            pltpu.VMEM((maps, rows, width), jnp.float32),
            pltpu.VMEM((maps, rows, 2 * width), jnp.float32),
        ],
        cost_estimate=pl.CostEstimate(
            flops=maps * rows * keys * 3 * width * 2,
            bytes_accessed=keys * 2 * width * 2,
            transcendentals=maps * rows * keys,
        ),
        compiler_params=pltpu.CompilerParams(vmem_limit_bytes=40 * 1024 * 1024),
        name="attention",
    )(place.reshape(1), attn_lambda, queries.reshape(rows, heads * width), head_gain.reshape(1, -1), *pieces)


def hidden_body(rows_hbm, *refs, shards):
    weight_refs = refs[: 2 * shards]
    out_ref, rows_ref, weights_ref, rows_sem, sems = refs[2 * shards :]
    rows_copy = pltpu.make_async_copy(rows_hbm, rows_ref, rows_sem)
    rows_copy.start()
    copies = [pltpu.make_async_copy(weight_refs[i], weights_ref.at[i], sems.at[i]) for i in range(2 * shards)]
    for copy in copies:
        copy.start()
    count = rows_ref.shape[0]
    block = count // 2
    rows_copy.wait()
    for shard in range(shards):
        copies[2 * shard].wait()
        copies[2 * shard + 1].wait()

        @pl.loop(0, count // block)
        def _(step):
            start = pl.multiple_of(step * block, block)
            rows = rows_ref[pl.ds(start, block), :]
            gate_out = jnp.dot(rows, weights_ref[2 * shard], preferred_element_type=jnp.float32)
            up_out = jnp.dot(rows, weights_ref[2 * shard + 1], preferred_element_type=jnp.float32)
            out_ref[shard, pl.ds(start, block), :] = (jax.nn.silu(gate_out) * up_out).astype(jnp.bfloat16)


def hidden_units(rows, weights):
    count, depth = rows.shape
    units = weights[0][0].shape[1]
    shards = len(weights)
    flat = [w for pair in weights for w in pair]
    return pl.pallas_call(
        functools.partial(hidden_body, shards=shards),
        out_shape=jax.ShapeDtypeStruct((shards, count, units), jnp.bfloat16),
        in_specs=[pl.BlockSpec(memory_space=pltpu.HBM)] * (1 + len(flat)),
        out_specs=pl.BlockSpec(memory_space=pltpu.VMEM),
        scratch_shapes=[
            pltpu.VMEM((count, depth), jnp.bfloat16),
            pltpu.VMEM((len(flat), depth, units), jnp.bfloat16),
            pltpu.SemaphoreType.DMA,
            pltpu.SemaphoreType.DMA((len(flat),)),
        ],
        cost_estimate=pl.CostEstimate(
            flops=4 * count * depth * units * shards,
            bytes_accessed=2 * depth * (count + 2 * units * shards),
            transcendentals=count * units * shards,
        ),
        compiler_params=pltpu.CompilerParams(vmem_limit_bytes=32 * 1024 * 1024),
        name="hidden_units",
    )(rows, *flat)


def down_body(hidden_ref, *refs, parts, begun):
    hidden = jnp.concatenate([hidden_ref[k] for k in range(hidden_ref.shape[0])], axis=1)
    weights = jnp.concatenate([ref[...] for ref in refs[:parts]], axis=0)
    total = jnp.dot(hidden, weights, preferred_element_type=jnp.float32)
    if begun:
        total = total + refs[parts][...]
    refs[-1][...] = total.astype(refs[-1].dtype)


def down_product(hidden, shards, weights, begun, kind):
    _, rows, units = hidden.shape
    width = weights[0].shape[1]
    cols = width // 4
    depth = sum(w.shape[0] for w in weights)
    first = shards[0] // len(shards)
    return pl.pallas_call(
        functools.partial(down_body, parts=len(weights), begun=len(begun)),
        grid=(width // cols,),
        out_shape=jax.ShapeDtypeStruct((rows, width), kind),
        in_specs=[pl.BlockSpec((len(shards), rows, units), lambda n: (first, 0, 0))]
        + [pl.BlockSpec((w.shape[0], cols), lambda n: (0, n)) for w in weights]
        + [pl.BlockSpec((rows, cols), lambda n: (0, n)) for _ in begun],
        out_specs=pl.BlockSpec((rows, cols), lambda n: (0, n)),
        cost_estimate=pl.CostEstimate(
            flops=2 * rows * width * depth, bytes_accessed=4 * rows * width, transcendentals=0
        ),
        name="down_product",
    )(hidden, *weights, *begun)


def ring(size, step):
    return [(i, (i + step) % size) for i in range(size)]


def local(
    queries,
    keys,
    values,
    attn_lambda,
    head_gain,
    w_out,
    moe_rows,
    moe_gain,
    routes,
    route_weights,
    w_gate,
    w_up,
    w_down,
):
    tp_count = lax.axis_size("tp")
    tp_id = lax.axis_index("tp")
    experts = lax.axis_size("ep")
    positions, _, _ = queries.shape
    model_width = moe_rows.shape[1]
    dev_rows = moe_rows.shape[0] // tp_count
    top_count = routes.shape[1]
    capacity = max(2, 2 * dev_rows * top_count // experts)
    slots = experts * capacity
    up_ring, down_ring = ring(tp_count, 1), ring(tp_count, -1)

    gate, up = w_gate[0], w_up[0]
    half = w_down.shape[1] // 2
    down = w_down[0]
    downs = [down[:half], down[half:]]

    def send(x, way):
        return lax.ppermute(x, "tp", way)

    gate_a, gate_b = send(gate, up_ring), send(gate, down_ring)
    up_a, up_b = send(up, up_ring), send(up, down_ring)
    gate_c, up_c = send(gate_a, up_ring), send(up_b, down_ring)
    down_parts = []
    for c, x in enumerate(downs):
        near_a, near_b = send(x, up_ring), send(x, down_ring)
        far = send(near_a, up_ring) if c == 0 else send(near_b, down_ring)
        down_parts.append((near_a, near_b, far))

    z_size, x_size, cores = EP_SIZES

    def ep_shift(dz, dx, dc):
        pairs = []
        for i in range(experts):
            z, x, c = i // (x_size * cores), i // cores % x_size, i % cores
            to = ((z + dz) % z_size * x_size + (x + dx) % x_size) * cores + (c + dc) % cores
            pairs.append((i, to))
        return pairs

    def spread(x, shift):
        return lax.ppermute(x, "ep", ep_shift(*shift))

    kv = jnp.concatenate([keys.reshape(positions, -1), values.reshape(positions, -1)], axis=1)
    column = jnp.concatenate([kv] + [spread(kv, (d, 0, 0)) for d in range(1, z_size)], axis=0)
    own_pieces = [column] + [spread(column, (0, d, 0)) for d in range(1, x_size)]
    other_pieces = [spread(piece, (0, 0, 1)) for piece in own_pieces]

    own_routes = lax.dynamic_slice_in_dim(routes, tp_id * dev_rows, dev_rows, 0)
    own_weights = lax.dynamic_slice_in_dim(route_weights, tp_id * dev_rows, dev_rows, 0)
    rows_f = lax.dynamic_slice_in_dim(moe_rows, tp_id * dev_rows, dev_rows, 0).astype(jnp.float32)
    mean_sq = jnp.mean(rows_f * rows_f, axis=-1, keepdims=True)
    normed = (rows_f * lax.rsqrt(mean_sq + EPSILON) * moe_gain).astype(jnp.bfloat16)
    flat_ids = own_routes.reshape(-1)
    order = lax.iota(jnp.int32, flat_ids.shape[0])
    same = (flat_ids[:, None] == flat_ids[None, :]) & (order[None, :] < order[:, None])
    slot_ids = jnp.sum(same.astype(jnp.int32), axis=1)
    place = (flat_ids * capacity + slot_ids).reshape(dev_rows, top_count)
    slot_range = lax.iota(jnp.int32, slots)
    taken = slot_range[:, None] == place[:, 0][None, :]
    for k in range(1, top_count):
        taken = taken | (slot_range[:, None] == place[:, k][None, :])
    outgoing = jnp.dot(taken.astype(jnp.bfloat16), normed, preferred_element_type=jnp.float32).astype(jnp.bfloat16)
    arrived = lax.all_to_all(
        outgoing.reshape(experts, capacity, model_width), "ep", split_axis=0, concat_axis=0, tiled=True
    ).reshape(slots, model_width)

    hidden = hidden_units(arrived, [(gate, up), (gate_a, up_a), (gate_b, up_b), (gate_c, up_c)])

    hit = [(slot_range[None, :] == place[:, k][:, None]).astype(jnp.float32) for k in range(top_count)]
    mix = sum(own_weights[:, k : k + 1] * hit[k] for k in range(top_count))
    near_a, near_b, far = zip(*down_parts)
    begun = down_product(hidden, (0, 1, 2), [down, *near_a, *near_b], [], jnp.float32)
    out = down_product(hidden, (3,), far, [begun], jnp.bfloat16)
    returned = lax.all_to_all(
        out.reshape(experts, capacity, -1), "ep", split_axis=0, concat_axis=0, tiled=True
    ).reshape(slots, -1)
    moe_out = jnp.dot(mix.astype(jnp.bfloat16), returned, preferred_element_type=jnp.float32).astype(jnp.bfloat16)

    attn_rows = attention(queries, own_pieces + other_pieces, attn_lambda, head_gain, lax.axis_index("ep"))
    block = positions // tp_count
    head_width = attn_rows.shape[1]
    mixer_f = jnp.zeros((block, model_width), jnp.float32)
    for step in range(tp_count):
        piece = lax.dynamic_slice_in_dim(attn_rows, (tp_id + step) % tp_count * block, block, 0)
        if step:
            piece = send(piece, ring(tp_count, step))
        w_rows = lax.dynamic_slice_in_dim(w_out, (tp_id - step) % tp_count * head_width, head_width, 0)
        mixer_f = mixer_f + jnp.dot(piece, w_rows, preferred_element_type=jnp.float32)
    mixer_out = mixer_f.astype(jnp.bfloat16)
    return (mixer_out, moe_out)


def solution(mesh):
    return jax.shard_map(
        local,
        mesh=mesh,
        in_specs=(
            P("ep", "tp", None),
            P("ep", "tp", None),
            P("ep", "tp", None),
            P("tp"),
            P(),
            P(),
            P("ep", None),
            P(),
            P("ep", None),
            P("ep", None),
            P("ep", None, "tp"),
            P("ep", None, "tp"),
            P("ep", "tp", None),
        ),
        out_specs=(P(("ep", "tp"), None), P(("ep", "tp"), None)),
        check_vma=False,
    )
```

```python
import functools

import jax
import jax.numpy as jnp
from jax import lax
from jax.experimental import pallas as pl
from jax.experimental.pallas import tpu as pltpu
from jax.sharding import PartitionSpec as P


EPSILON = 1e-06
MASKED = -1e30
WHOLE_VMEM = 60 * 1024 * 1024
EP_SIZES = (8, 4, 2)


def attention_body(place_ref, lam_ref, q_ref, gain_ref, *refs, heads, dim):
    _, x_size, cores = EP_SIZES
    count = x_size * cores
    piece_refs = refs[:count]
    out_ref, kv_ref, sems, qs_ref, max_ref, acc_ref = refs[count:]
    copies = [pltpu.make_async_copy(piece_refs[i], kv_ref.at[i], sems.at[i]) for i in range(count)]
    for copy in copies:
        copy.start()
    rows = q_ref.shape[0]
    width = 2 * dim
    me = place_ref[0]
    core = me % cores
    x = (me // cores) % x_size
    z = me // (cores * x_size)
    lane = lax.broadcasted_iota(jnp.int32, (rows, width), 1)
    for h in range(heads):
        q_h = q_ref[:, h * width : (h + 1) * width] * jnp.bfloat16(dim**-0.5)
        for m in range(2):
            qs_ref[2 * h + m] = jnp.where((lane >= m * dim) & (lane < (m + 1) * dim), q_h, jnp.bfloat16(0))
    max_ref[...] = jnp.full_like(max_ref, MASKED)
    acc_ref[...] = jnp.zeros_like(acc_ref)
    for copy in copies:
        copy.wait()

    def visit(pieces, offset, places):
        key_blk = jnp.concatenate([kv_ref[p, pl.ds(offset, rows), :width] for p in pieces], axis=0)
        value_blk = jnp.concatenate([kv_ref[p, pl.ds(offset, rows), width:] for p in pieces], axis=0)
        value_ones = jnp.concatenate([value_blk, jnp.ones_like(value_blk)], axis=1)
        for g in range(2 * heads):
            scores = lax.dot_general(
                qs_ref[g], key_blk, (((1,), (1,)), ((), ())), preferred_element_type=jnp.float32
            )
            if places is not None:
                shape = (rows, rows)
                query_pos = me * rows + lax.broadcasted_iota(jnp.int32, shape, 0)
                key_pos = lax.broadcasted_iota(jnp.int32, shape, 1)
                first_key = jnp.concatenate([place * rows + key_pos for place in places], axis=1)
                allowed = first_key <= jnp.concatenate([query_pos] * len(places), axis=1)
                scores = jnp.where(allowed, scores, MASKED)
            old_max = max_ref[g]
            new_max = jnp.maximum(old_max, jnp.max(scores, axis=1, keepdims=True))
            shrink = jnp.exp(old_max - new_max)
            spread_max = jnp.concatenate([new_max] * (scores.shape[1] // width), axis=1)
            weights = jnp.exp(scores - spread_max).astype(jnp.bfloat16)
            part = jnp.dot(weights, value_ones, preferred_element_type=jnp.float32)
            acc_ref[g] = acc_ref[g] * jnp.concatenate([shrink, shrink], axis=1) + part
            max_ref[g] = new_max

    @pl.loop(0, x + 1)
    def _(dx):
        first = (z * x_size + x - dx) * cores
        visit((dx, x_size + dx), 0, (first + core, first + 1 - core))

    @pl.loop(0, z * cores)
    def _(step):
        offset = pl.multiple_of((step // cores + 1) * rows, rows)
        first = step % cores * x_size
        visit([first + dx for dx in range(x_size)], offset, None)

    for h in range(heads):
        one, two = acc_ref[2 * h], acc_ref[2 * h + 1]
        head_out = one[:, :width] / one[:, width:] - lam_ref[h] * (two[:, :width] / two[:, width:])
        mean_sq = jnp.mean(head_out * head_out, axis=1, keepdims=True)
        out_ref[:, h * width : (h + 1) * width] = (
            head_out * lax.rsqrt(mean_sq + EPSILON) * gain_ref[...]
        ).astype(jnp.bfloat16)


def attention(queries, pieces, attn_lambda, head_gain, place):
    rows, heads, width = queries.shape
    maps = 2 * heads
    count = len(pieces)
    keys = count * pieces[0].shape[0]
    return pl.pallas_call(
        functools.partial(attention_body, heads=heads, dim=width // 2),
        out_shape=jax.ShapeDtypeStruct((rows, heads * width), jnp.bfloat16),
        in_specs=[pl.BlockSpec(memory_space=pltpu.SMEM)] * 2
        + [pl.BlockSpec(memory_space=pltpu.VMEM)] * 2
        + [pl.BlockSpec(memory_space=pltpu.HBM)] * count,
        out_specs=pl.BlockSpec(memory_space=pltpu.VMEM),
        scratch_shapes=[
            pltpu.VMEM((count, *pieces[0].shape), jnp.bfloat16),
            pltpu.SemaphoreType.DMA((count,)),
            pltpu.VMEM((maps, rows, width), jnp.bfloat16),
            pltpu.VMEM((maps, rows, width), jnp.float32),
            pltpu.VMEM((maps, rows, 2 * width), jnp.float32),
        ],
        cost_estimate=pl.CostEstimate(
            flops=maps * rows * keys * 3 * width * 2,
            bytes_accessed=keys * 2 * width * 2,
            transcendentals=maps * rows * keys,
        ),
        compiler_params=pltpu.CompilerParams(vmem_limit_bytes=40 * 1024 * 1024),
        name="attention",
    )(place.reshape(1), attn_lambda, queries.reshape(rows, heads * width), head_gain.reshape(1, -1), *pieces)


def hidden_body(rows_hbm, *refs, shards):
    weight_refs = refs[: 2 * shards]
    out_ref, rows_ref, weights_ref, rows_sem, sems = refs[2 * shards :]
    rows_copy = pltpu.make_async_copy(rows_hbm, rows_ref, rows_sem)
    rows_copy.start()
    for i in range(2 * shards):
        pltpu.make_async_copy(weight_refs[i], weights_ref.at[i], sems.at[i]).start()
    rows_copy.wait()

    @pl.loop(0, shards)
    def _(shard):
        for i in range(2):
            at = 2 * shard + i
            pltpu.make_async_copy(weight_refs[i], weights_ref.at[at], sems.at[at]).wait()
        rows = rows_ref[...]
        gate_out = jnp.dot(rows, weights_ref[2 * shard], preferred_element_type=jnp.float32)
        up_out = jnp.dot(rows, weights_ref[2 * shard + 1], preferred_element_type=jnp.float32)
        out_ref[shard] = (jax.nn.silu(gate_out) * up_out).astype(jnp.bfloat16)


def hidden_units(rows, weights):
    count, depth = rows.shape
    units = weights[0][0].shape[1]
    shards = len(weights)
    flat = [w for pair in weights for w in pair]
    return pl.pallas_call(
        functools.partial(hidden_body, shards=shards),
        out_shape=jax.ShapeDtypeStruct((shards, count, units), jnp.bfloat16),
        in_specs=[pl.BlockSpec(memory_space=pltpu.HBM)] * (1 + len(flat)),
        out_specs=pl.BlockSpec(memory_space=pltpu.VMEM),
        scratch_shapes=[
            pltpu.VMEM((count, depth), jnp.bfloat16),
            pltpu.VMEM((len(flat), depth, units), jnp.bfloat16),
            pltpu.SemaphoreType.DMA,
            pltpu.SemaphoreType.DMA((len(flat),)),
        ],
        cost_estimate=pl.CostEstimate(
            flops=4 * count * depth * units * shards,
            bytes_accessed=2 * depth * (count + 2 * units * shards),
            transcendentals=count * units * shards,
        ),
        compiler_params=pltpu.CompilerParams(vmem_limit_bytes=WHOLE_VMEM),
        name="hidden_units",
    )(rows, *flat)


def down_body(hidden_ref, *refs, parts, begun):
    hidden = jnp.concatenate([hidden_ref[k] for k in range(hidden_ref.shape[0])], axis=1)
    weights = jnp.concatenate([ref[...] for ref in refs[:parts]], axis=0)
    total = jnp.dot(hidden, weights, preferred_element_type=jnp.float32)
    if begun:
        total = total + refs[parts][...]
    refs[-1][...] = total.astype(refs[-1].dtype)


def down_product(hidden, shards, weights, begun, kind):
    _, rows, units = hidden.shape
    width = weights[0].shape[1]
    cols = width // 4
    depth = sum(w.shape[0] for w in weights)
    first = shards[0] // len(shards)
    return pl.pallas_call(
        functools.partial(down_body, parts=len(weights), begun=len(begun)),
        grid=(width // cols,),
        out_shape=jax.ShapeDtypeStruct((rows, width), kind),
        in_specs=[pl.BlockSpec((len(shards), rows, units), lambda n: (first, 0, 0))]
        + [pl.BlockSpec((w.shape[0], cols), lambda n: (0, n)) for w in weights]
        + [pl.BlockSpec((rows, cols), lambda n: (0, n)) for _ in begun],
        out_specs=pl.BlockSpec((rows, cols), lambda n: (0, n)),
        cost_estimate=pl.CostEstimate(
            flops=2 * rows * width * depth, bytes_accessed=4 * rows * width, transcendentals=0
        ),
        compiler_params=pltpu.CompilerParams(vmem_limit_bytes=WHOLE_VMEM),
        name="down_product",
    )(hidden, *weights, *begun)


def ring(size, step):
    return [(i, (i + step) % size) for i in range(size)]


def local(
    queries,
    keys,
    values,
    attn_lambda,
    head_gain,
    w_out,
    moe_rows,
    moe_gain,
    routes,
    route_weights,
    w_gate,
    w_up,
    w_down,
):
    tp_count = lax.axis_size("tp")
    tp_id = lax.axis_index("tp")
    experts = lax.axis_size("ep")
    positions, _, _ = queries.shape
    model_width = moe_rows.shape[1]
    dev_rows = moe_rows.shape[0] // tp_count
    top_count = routes.shape[1]
    capacity = max(2, 2 * dev_rows * top_count // experts)
    slots = experts * capacity
    up_ring, down_ring = ring(tp_count, 1), ring(tp_count, -1)

    gate, up = w_gate[0], w_up[0]
    half = w_down.shape[1] // 2
    down = w_down[0]
    downs = [down[:half], down[half:]]

    def send(x, way):
        return lax.ppermute(x, "tp", way)

    gate_a, gate_b = send(gate, up_ring), send(gate, down_ring)
    up_a, up_b = send(up, up_ring), send(up, down_ring)
    gate_c, up_c = send(gate_a, up_ring), send(up_b, down_ring)
    down_parts = []
    for c, x in enumerate(downs):
        near_a, near_b = send(x, up_ring), send(x, down_ring)
        far = send(near_a, up_ring) if c == 0 else send(near_b, down_ring)
        down_parts.append((near_a, near_b, far))

    z_size, x_size, cores = EP_SIZES

    def ep_shift(dz, dx, dc):
        pairs = []
        for i in range(experts):
            z, x, c = i // (x_size * cores), i // cores % x_size, i % cores
            to = ((z + dz) % z_size * x_size + (x + dx) % x_size) * cores + (c + dc) % cores
            pairs.append((i, to))
        return pairs

    def spread(x, shift):
        return lax.ppermute(x, "ep", ep_shift(*shift))

    kv = jnp.concatenate([keys.reshape(positions, -1), values.reshape(positions, -1)], axis=1)
    column = jnp.concatenate([kv] + [spread(kv, (d, 0, 0)) for d in range(1, z_size)], axis=0)
    own_pieces = [column] + [spread(column, (0, d, 0)) for d in range(1, x_size)]
    other_pieces = [spread(piece, (0, 0, 1)) for piece in own_pieces]

    own_routes = lax.dynamic_slice_in_dim(routes, tp_id * dev_rows, dev_rows, 0)
    own_weights = lax.dynamic_slice_in_dim(route_weights, tp_id * dev_rows, dev_rows, 0)
    rows_f = lax.dynamic_slice_in_dim(moe_rows, tp_id * dev_rows, dev_rows, 0).astype(jnp.float32)
    mean_sq = jnp.mean(rows_f * rows_f, axis=-1, keepdims=True)
    normed = (rows_f * lax.rsqrt(mean_sq + EPSILON) * moe_gain).astype(jnp.bfloat16)
    flat_ids = own_routes.reshape(-1)
    order = lax.iota(jnp.int32, flat_ids.shape[0])
    same = (flat_ids[:, None] == flat_ids[None, :]) & (order[None, :] < order[:, None])
    slot_ids = jnp.sum(same.astype(jnp.int32), axis=1)
    place = (flat_ids * capacity + slot_ids).reshape(dev_rows, top_count)
    slot_range = lax.iota(jnp.int32, slots)
    taken = slot_range[:, None] == place[:, 0][None, :]
    for k in range(1, top_count):
        taken = taken | (slot_range[:, None] == place[:, k][None, :])
    outgoing = jnp.dot(taken.astype(jnp.bfloat16), normed, preferred_element_type=jnp.float32).astype(jnp.bfloat16)
    arrived = lax.all_to_all(
        outgoing.reshape(experts, capacity, model_width), "ep", split_axis=0, concat_axis=0, tiled=True
    ).reshape(slots, model_width)

    hidden = hidden_units(arrived, [(gate, up), (gate_a, up_a), (gate_b, up_b), (gate_c, up_c)])

    hit = [(slot_range[None, :] == place[:, k][:, None]).astype(jnp.float32) for k in range(top_count)]
    mix = sum(own_weights[:, k : k + 1] * hit[k] for k in range(top_count))
    near_a, near_b, far = zip(*down_parts)
    begun = down_product(hidden, (0, 1, 2), [down, *near_a, *near_b], [], jnp.float32)
    out = down_product(hidden, (3,), far, [begun], jnp.bfloat16)
    returned = lax.all_to_all(
        out.reshape(experts, capacity, -1), "ep", split_axis=0, concat_axis=0, tiled=True
    ).reshape(slots, -1)
    moe_out = jnp.dot(mix.astype(jnp.bfloat16), returned, preferred_element_type=jnp.float32).astype(jnp.bfloat16)

    attn_rows = attention(queries, own_pieces + other_pieces, attn_lambda, head_gain, lax.axis_index("ep"))
    block = positions // tp_count
    head_width = attn_rows.shape[1]
    mixer_f = jnp.zeros((block, model_width), jnp.float32)
    for step in range(tp_count):
        piece = lax.dynamic_slice_in_dim(attn_rows, (tp_id + step) % tp_count * block, block, 0)
        if step:
            piece = send(piece, ring(tp_count, step))
        w_rows = lax.dynamic_slice_in_dim(w_out, (tp_id - step) % tp_count * head_width, head_width, 0)
        mixer_f = mixer_f + jnp.dot(piece, w_rows, preferred_element_type=jnp.float32)
    mixer_out = mixer_f.astype(jnp.bfloat16)
    return (mixer_out, moe_out)


def solution(mesh):
    return jax.shard_map(
        local,
        mesh=mesh,
        in_specs=(
            P("ep", "tp", None),
            P("ep", "tp", None),
            P("ep", "tp", None),
            P("tp"),
            P(),
            P(),
            P("ep", None),
            P(),
            P("ep", None),
            P("ep", None),
            P("ep", None, "tp"),
            P("ep", None, "tp"),
            P("ep", "tp", None),
        ),
        out_specs=(P(("ep", "tp"), None), P(("ep", "tp"), None)),
        check_vma=False,
    )
```

```python
import functools

import jax
import jax.numpy as jnp
from jax import lax
from jax.experimental import pallas as pl
from jax.experimental.pallas import tpu as pltpu
from jax.sharding import PartitionSpec as P


EPSILON = 1e-06
MASKED = -1e30
COPY_PARTS = 4
WHOLE_VMEM = 60 * 1024 * 1024
EP_SIZES = (8, 4, 2)


def attention_body(place_ref, lam_ref, q_ref, gain_ref, *refs, heads, dim):
    _, x_size, cores = EP_SIZES
    count = x_size * cores
    piece_refs = refs[:count]
    out_ref, kv_ref, sems, qs_ref, max_ref, acc_ref = refs[count:]
    copies = [pltpu.make_async_copy(piece_refs[i], kv_ref.at[i], sems.at[i]) for i in range(count)]
    for copy in copies:
        copy.start()
    rows = q_ref.shape[0]
    width = 2 * dim
    me = place_ref[0]
    core = me % cores
    x = (me // cores) % x_size
    z = me // (cores * x_size)
    lane = lax.broadcasted_iota(jnp.int32, (rows, width), 1)
    for h in range(heads):
        q_h = q_ref[:, h * width : (h + 1) * width] * jnp.bfloat16(dim**-0.5)
        for m in range(2):
            qs_ref[2 * h + m] = jnp.where((lane >= m * dim) & (lane < (m + 1) * dim), q_h, jnp.bfloat16(0))
    max_ref[...] = jnp.full_like(max_ref, MASKED)
    acc_ref[...] = jnp.zeros_like(acc_ref)
    for copy in copies:
        copy.wait()

    def visit(pieces, offset, places):
        key_blk = jnp.concatenate([kv_ref[p, pl.ds(offset, rows), :width] for p in pieces], axis=0)
        value_blk = jnp.concatenate([kv_ref[p, pl.ds(offset, rows), width:] for p in pieces], axis=0)
        value_ones = jnp.concatenate([value_blk, jnp.ones_like(value_blk)], axis=1)
        for g in range(2 * heads):
            scores = lax.dot_general(
                qs_ref[g], key_blk, (((1,), (1,)), ((), ())), preferred_element_type=jnp.float32
            )
            if places is not None:
                shape = (rows, rows)
                query_pos = me * rows + lax.broadcasted_iota(jnp.int32, shape, 0)
                key_pos = lax.broadcasted_iota(jnp.int32, shape, 1)
                first_key = jnp.concatenate([place * rows + key_pos for place in places], axis=1)
                allowed = first_key <= jnp.concatenate([query_pos] * len(places), axis=1)
                scores = jnp.where(allowed, scores, MASKED)
            old_max = max_ref[g]
            new_max = jnp.maximum(old_max, jnp.max(scores, axis=1, keepdims=True))
            shrink = jnp.exp(old_max - new_max)
            spread_max = jnp.concatenate([new_max] * (scores.shape[1] // width), axis=1)
            weights = jnp.exp(scores - spread_max).astype(jnp.bfloat16)
            part = jnp.dot(weights, value_ones, preferred_element_type=jnp.float32)
            acc_ref[g] = acc_ref[g] * jnp.concatenate([shrink, shrink], axis=1) + part
            max_ref[g] = new_max

    @pl.loop(0, x + 1)
    def _(dx):
        first = (z * x_size + x - dx) * cores
        visit((dx, x_size + dx), 0, (first + core, first + 1 - core))

    @pl.loop(0, z * cores)
    def _(step):
        offset = pl.multiple_of((step // cores + 1) * rows, rows)
        first = step % cores * x_size
        visit([first + dx for dx in range(x_size)], offset, None)

    for h in range(heads):
        one, two = acc_ref[2 * h], acc_ref[2 * h + 1]
        head_out = one[:, :width] / one[:, width:] - lam_ref[h] * (two[:, :width] / two[:, width:])
        mean_sq = jnp.mean(head_out * head_out, axis=1, keepdims=True)
        out_ref[:, h * width : (h + 1) * width] = (
            head_out * lax.rsqrt(mean_sq + EPSILON) * gain_ref[...]
        ).astype(jnp.bfloat16)


def attention(queries, pieces, attn_lambda, head_gain, place):
    rows, heads, width = queries.shape
    maps = 2 * heads
    count = len(pieces)
    keys = count * pieces[0].shape[0]
    return pl.pallas_call(
        functools.partial(attention_body, heads=heads, dim=width // 2),
        out_shape=jax.ShapeDtypeStruct((rows, heads * width), jnp.bfloat16),
        in_specs=[pl.BlockSpec(memory_space=pltpu.SMEM)] * 2
        + [pl.BlockSpec(memory_space=pltpu.VMEM)] * 2
        + [pl.BlockSpec(memory_space=pltpu.HBM)] * count,
        out_specs=pl.BlockSpec(memory_space=pltpu.VMEM),
        scratch_shapes=[
            pltpu.VMEM((count, *pieces[0].shape), jnp.bfloat16),
            pltpu.SemaphoreType.DMA((count,)),
            pltpu.VMEM((maps, rows, width), jnp.bfloat16),
            pltpu.VMEM((maps, rows, width), jnp.float32),
            pltpu.VMEM((maps, rows, 2 * width), jnp.float32),
        ],
        cost_estimate=pl.CostEstimate(
            flops=maps * rows * keys * 3 * width * 2,
            bytes_accessed=keys * 2 * width * 2,
            transcendentals=maps * rows * keys,
        ),
        compiler_params=pltpu.CompilerParams(vmem_limit_bytes=40 * 1024 * 1024),
        name="attention",
    )(place.reshape(1), attn_lambda, queries.reshape(rows, heads * width), head_gain.reshape(1, -1), *pieces)


def hidden_body(rows_hbm, *refs, shards):
    weight_refs = refs[: 2 * shards]
    out_ref, rows_ref, weights_ref, rows_sem, sems = refs[2 * shards :]

    def start_copies(source, target, sem):
        part = source.shape[0] // COPY_PARTS
        for n in range(COPY_PARTS):
            at = pl.ds(n * part, part)
            pltpu.make_async_copy(source.at[at], target.at[at], sem).start()

    start_copies(rows_hbm, rows_ref, rows_sem)
    units = out_ref.shape[2]
    sides = [pl.ds(i * units, units) for i in range(2)]
    for i in range(2 * shards):
        start_copies(weight_refs[i], weights_ref.at[i // 2, :, sides[i % 2]], sems.at[i])
    pltpu.make_async_copy(rows_hbm, rows_ref, rows_sem).wait()

    @pl.loop(0, shards)
    def _(shard):
        for i in range(2):
            pltpu.make_async_copy(
                weight_refs[i], weights_ref.at[shard, :, sides[i]], sems.at[2 * shard + i]
            ).wait()
        both = jnp.dot(rows_ref[...], weights_ref[shard], preferred_element_type=jnp.float32)
        out_ref[shard] = (jax.nn.silu(both[:, :units]) * both[:, units:]).astype(jnp.bfloat16)


def hidden_units(rows, weights):
    count, depth = rows.shape
    units = weights[0][0].shape[1]
    shards = len(weights)
    flat = [w for pair in weights for w in pair]
    return pl.pallas_call(
        functools.partial(hidden_body, shards=shards),
        out_shape=jax.ShapeDtypeStruct((shards, count, units), jnp.bfloat16),
        in_specs=[pl.BlockSpec(memory_space=pltpu.HBM)] * (1 + len(flat)),
        out_specs=pl.BlockSpec(memory_space=pltpu.VMEM),
        scratch_shapes=[
            pltpu.VMEM((count, depth), jnp.bfloat16),
            pltpu.VMEM((shards, depth, 2 * units), jnp.bfloat16),
            pltpu.SemaphoreType.DMA,
            pltpu.SemaphoreType.DMA((len(flat),)),
        ],
        cost_estimate=pl.CostEstimate(
            flops=4 * count * depth * units * shards,
            bytes_accessed=2 * depth * (count + 2 * units * shards),
            transcendentals=count * units * shards,
        ),
        compiler_params=pltpu.CompilerParams(vmem_limit_bytes=WHOLE_VMEM),
        name="hidden_units",
    )(rows, *flat)


def down_body(hidden_ref, *refs):
    hidden = jnp.concatenate([hidden_ref[k] for k in range(hidden_ref.shape[0])], axis=1)
    weights = jnp.concatenate([ref[...] for ref in refs[:-1]], axis=0)
    refs[-1][...] = jnp.dot(hidden, weights, preferred_element_type=jnp.float32).astype(refs[-1].dtype)


def down_product(hidden, shards, weights):
    rows, units = hidden.shape[1:]
    width = weights[0].shape[1]
    cols = width // 4
    depth = sum(w.shape[0] for w in weights)
    return pl.pallas_call(
        down_body,
        grid=(width // cols,),
        out_shape=jax.ShapeDtypeStruct((rows, width), jnp.bfloat16),
        in_specs=[pl.BlockSpec((shards, rows, units), lambda n: (0, 0, 0))]
        + [pl.BlockSpec((w.shape[0], cols), lambda n: (0, n)) for w in weights],
        out_specs=pl.BlockSpec((rows, cols), lambda n: (0, n)),
        cost_estimate=pl.CostEstimate(
            flops=2 * rows * width * depth, bytes_accessed=4 * rows * width, transcendentals=0
        ),
        compiler_params=pltpu.CompilerParams(vmem_limit_bytes=WHOLE_VMEM),
        name="down_product",
    )(hidden, *weights)


def finish_body(hidden_hbm, top_hbm, bottom_hbm, begun_hbm, out_hbm, hidden_ref, weights_ref, begun_ref, out_ref, sems, in_sems, out_sems):
    half = top_hbm.shape[0]
    loads = [
        pltpu.make_async_copy(hidden_hbm.at[hidden_hbm.shape[0] - 1], hidden_ref, sems.at[0]),
        pltpu.make_async_copy(top_hbm, weights_ref.at[pl.ds(0, half)], sems.at[1]),
        pltpu.make_async_copy(bottom_hbm, weights_ref.at[pl.ds(half, half)], sems.at[2]),
    ]
    for load in loads:
        load.start()
    count = in_sems.shape[0]
    cols = out_ref.shape[1] // count
    chunks = [pl.ds(n * cols, cols) for n in range(count)]
    begun = [pltpu.make_async_copy(begun_hbm.at[:, at], begun_ref.at[:, at], in_sems.at[n]) for n, at in enumerate(chunks)]
    made = [pltpu.make_async_copy(out_ref.at[:, at], out_hbm.at[:, at], out_sems.at[n]) for n, at in enumerate(chunks)]
    for copy in begun:
        copy.start()
    for load in loads:
        load.wait()
    for n, at in enumerate(chunks):
        total = jnp.dot(hidden_ref[...], weights_ref[:, at], preferred_element_type=jnp.float32)
        begun[n].wait()
        out_ref[:, at] = (total + begun_ref[:, at].astype(jnp.float32)).astype(jnp.bfloat16)
        made[n].start()
    for copy in made:
        copy.wait()


def finish_product(hidden, top, bottom, begun):
    rows, width = begun.shape
    units = hidden.shape[2]
    count = 4
    return pl.pallas_call(
        finish_body,
        out_shape=jax.ShapeDtypeStruct((rows, width), jnp.bfloat16),
        in_specs=[pl.BlockSpec(memory_space=pltpu.HBM)] * 4,
        out_specs=pl.BlockSpec(memory_space=pltpu.HBM),
        scratch_shapes=[
            pltpu.VMEM((rows, units), jnp.bfloat16),
            pltpu.VMEM((units, width), jnp.bfloat16),
            pltpu.VMEM((rows, width), jnp.bfloat16),
            pltpu.VMEM((rows, width), jnp.bfloat16),
            pltpu.SemaphoreType.DMA((3,)),
            pltpu.SemaphoreType.DMA((count,)),
            pltpu.SemaphoreType.DMA((count,)),
        ],
        cost_estimate=pl.CostEstimate(
            flops=2 * rows * width * units, bytes_accessed=4 * rows * width, transcendentals=0
        ),
        compiler_params=pltpu.CompilerParams(vmem_limit_bytes=WHOLE_VMEM),
        name="finish_product",
    )(hidden, top, bottom, begun)


def ring(size, step):
    return [(i, (i + step) % size) for i in range(size)]


def local(
    queries,
    keys,
    values,
    attn_lambda,
    head_gain,
    w_out,
    moe_rows,
    moe_gain,
    routes,
    route_weights,
    w_gate,
    w_up,
    w_down,
):
    tp_count = lax.axis_size("tp")
    tp_id = lax.axis_index("tp")
    experts = lax.axis_size("ep")
    positions, _, _ = queries.shape
    model_width = moe_rows.shape[1]
    dev_rows = moe_rows.shape[0] // tp_count
    top_count = routes.shape[1]
    capacity = max(2, 2 * dev_rows * top_count // experts)
    slots = experts * capacity
    up_ring, down_ring = ring(tp_count, 1), ring(tp_count, -1)

    gate, up = w_gate[0], w_up[0]
    half = w_down.shape[1] // 2
    down = w_down[0]
    downs = [down[:half], down[half:]]

    def send(x, way):
        return lax.ppermute(x, "tp", way)

    gate_a, gate_b = send(gate, up_ring), send(gate, down_ring)
    up_a, up_b = send(up, up_ring), send(up, down_ring)
    gate_c, up_c = send(gate_a, up_ring), send(up_b, down_ring)
    down_parts = []
    for c, x in enumerate(downs):
        near_a, near_b = send(x, up_ring), send(x, down_ring)
        far = send(near_a, up_ring) if c == 0 else send(near_b, down_ring)
        down_parts.append((near_a, near_b, far))

    z_size, x_size, cores = EP_SIZES

    def ep_shift(dz, dx, dc):
        pairs = []
        for i in range(experts):
            z, x, c = i // (x_size * cores), i // cores % x_size, i % cores
            to = ((z + dz) % z_size * x_size + (x + dx) % x_size) * cores + (c + dc) % cores
            pairs.append((i, to))
        return pairs

    def spread(x, shift):
        return lax.ppermute(x, "ep", ep_shift(*shift))

    kv = jnp.concatenate([keys.reshape(positions, -1), values.reshape(positions, -1)], axis=1)
    column = jnp.concatenate([kv] + [spread(kv, (d, 0, 0)) for d in range(1, z_size)], axis=0)
    own_pieces = [column] + [spread(column, (0, d, 0)) for d in (1, x_size - 1)]
    own_pieces.insert(2, spread(own_pieces[2], (0, x_size - 1, 0)))
    other_pieces = [spread(piece, (0, 0, 1)) for piece in own_pieces]

    own_routes = lax.dynamic_slice_in_dim(routes, tp_id * dev_rows, dev_rows, 0)
    own_weights = lax.dynamic_slice_in_dim(route_weights, tp_id * dev_rows, dev_rows, 0)
    rows_f = lax.dynamic_slice_in_dim(moe_rows, tp_id * dev_rows, dev_rows, 0).astype(jnp.float32)
    mean_sq = jnp.mean(rows_f * rows_f, axis=-1, keepdims=True)
    normed = (rows_f * lax.rsqrt(mean_sq + EPSILON) * moe_gain).astype(jnp.bfloat16)
    flat_ids = own_routes.reshape(-1)
    order = lax.iota(jnp.int32, flat_ids.shape[0])
    same = (flat_ids[:, None] == flat_ids[None, :]) & (order[None, :] < order[:, None])
    slot_ids = jnp.sum(same.astype(jnp.int32), axis=1)
    place = (flat_ids * capacity + slot_ids).reshape(dev_rows, top_count)
    slot_range = lax.iota(jnp.int32, slots)
    taken = slot_range[:, None] == place[:, 0][None, :]
    for k in range(1, top_count):
        taken = taken | (slot_range[:, None] == place[:, k][None, :])
    outgoing = jnp.dot(taken.astype(jnp.bfloat16), normed, preferred_element_type=jnp.float32).astype(jnp.bfloat16)
    arrived = lax.all_to_all(
        outgoing.reshape(experts, capacity, model_width), "ep", split_axis=0, concat_axis=0, tiled=True
    ).reshape(slots, model_width)

    hidden = hidden_units(arrived, [(gate, up), (gate_a, up_a), (gate_b, up_b), (gate_c, up_c)])

    hit = [(slot_range[None, :] == place[:, k][:, None]).astype(jnp.float32) for k in range(top_count)]
    mix = sum(own_weights[:, k : k + 1] * hit[k] for k in range(top_count))
    near_a, near_b, far = zip(*down_parts)
    begun = down_product(hidden, 3, [down, *near_a, *near_b])
    out = finish_product(hidden, *far, begun)
    returned = lax.all_to_all(
        out.reshape(experts, capacity, -1), "ep", split_axis=0, concat_axis=0, tiled=True
    ).reshape(slots, -1)
    moe_out = jnp.dot(lax.optimization_barrier(mix.astype(jnp.bfloat16)), returned, preferred_element_type=jnp.float32).astype(jnp.bfloat16)

    attn_rows = attention(queries, own_pieces + other_pieces, attn_lambda, head_gain, lax.axis_index("ep"))
    block = positions // tp_count
    head_width = attn_rows.shape[1]
    mixer_f = jnp.zeros((block, model_width), jnp.float32)
    for step in range(tp_count):
        piece = lax.dynamic_slice_in_dim(attn_rows, (tp_id + step) % tp_count * block, block, 0)
        if step:
            piece = send(piece, ring(tp_count, step))
        w_rows = lax.dynamic_slice_in_dim(w_out, (tp_id - step) % tp_count * head_width, head_width, 0)
        mixer_f = mixer_f + jnp.dot(piece, w_rows, preferred_element_type=jnp.float32)
    mixer_out = mixer_f.astype(jnp.bfloat16)
    return (mixer_out, moe_out)


def solution(mesh):
    return jax.shard_map(
        local,
        mesh=mesh,
        in_specs=(
            P("ep", "tp", None),
            P("ep", "tp", None),
            P("ep", "tp", None),
            P("tp"),
            P(),
            P(),
            P("ep", None),
            P(),
            P("ep", None),
            P("ep", None),
            P("ep", None, "tp"),
            P("ep", None, "tp"),
            P("ep", "tp", None),
        ),
        out_specs=(P(("ep", "tp"), None), P(("ep", "tp"), None)),
        check_vma=False,
    )
```
